32 devices in a mesh: tp: 8 (over z, y), dp: 4 (over x, core).
Axes of the slice: x: 2, y: 2, z: 4, core: 2. Of those that a mesh axis runs over, the one named last changes fastest.
Arguments:
- residual: bfloat16 [128, 4096], P(None, ('dp', 'tp')), may hold values from -50 to 50, as said below
- norm_gain: bfloat16 [2, 4096], P(None, ('dp', 'tp')), may hold values from 0.099609375 to 1.8984375
- w_query: bfloat16 [2, 4096, 4096], P(None, 'dp', 'tp'), may hold values from -0.09375 to 0.09375
- w_forget: bfloat16 [2, 4096, 4096], P(None, 'dp', 'tp'), may hold values from -0.09375 to 0.09375
- w_value: bfloat16 [2, 4096, 4096], P(None, 'dp', 'tp'), may hold values from -0.09375 to 0.09375
- w_output_gate: bfloat16 [2, 4096, 4096], P(None, 'dp', 'tp'), may hold values from -0.09375 to 0.09375
- lower_bound: float32 [2, 4096], P(None, 'tp'), may hold values from 0 to 0.9
- head_gain: bfloat16 [2, 4096], P(None, 'tp'), may hold values from 0.099609375 to 1.8984375
- w_out: bfloat16 [2, 4096, 4096], P(None, 'tp', 'dp'), may hold values from -0.125 to 0.125
- state: float32 [2, 128, 32, 128, 128], P(None, 'dp', 'tp'), may hold values from -2.4 to 2.4
Outputs:
- new_residual: bfloat16 [128, 4096], P(None, ('dp', 'tp'))
- new_state: float32 [2, 128, 32, 128, 128], P(None, 'dp', 'tp')
The draws below stay inside these ranges and needn't reach their ends.
Inputs may be any that keep to these rules, and one draw needn't show every extreme that they name: residual rows of normal entries, each group of 16 consecutive features with its own scale.
All inputs are finite; a program needn't handle non-finite values.
Results may differ from the reference program's by a relative error of at most 0.02.
Values may be sent and summed in bfloat16 or wider, within the bound.
A program may use at most 128 MiB of HBM per device.

```python
import jax
import jax.numpy as jnp
from jax import lax

D = 4096
HEADS = 32
HEAD_DIM = 128
BLOCKS = 2
BATCH = 128
C = 4096
N_DP = 4


def draw_residual(key, part):
    first, second, third = jax.random.split(key, 3)
    base = jnp.clip(jax.random.normal(first, (BATCH, D), jnp.float32), -5.0, 5.0)
    groups = jnp.exp(jax.random.uniform(second, (D // 16,), jnp.float32, -1.2, 1.2))
    columns = jnp.repeat(groups, 16)
    return (base * columns[None, :]).astype(jnp.bfloat16)


def spiked(values, key, source, target, blocks, factor):
    def block_of(dim):
        return (jnp.arange(values.shape[dim]) // (values.shape[dim] // blocks)).reshape((-1,) + (1,) * (values.ndim - 1 - dim))

    near = jax.random.permutation(key, blocks)[block_of(target)]
    second = (block_of(target) + blocks // 2) % blocks
    return jnp.where((block_of(source) == near) | (block_of(source) == second), factor * values, values)


def levels(stream_key, shape, cuts, least, top_value):
    factor_of, own = 1.0, jax.random.fold_in(stream_key, 6)
    for dim, blocks in cuts:
        steps = jnp.exp(jax.random.uniform(jax.random.fold_in(own, dim), (blocks,), jnp.float32, least / len(cuts), top_value / len(cuts)))
        factor_of = factor_of * jnp.repeat(steps, shape[dim] // blocks).reshape([-1 if axis == dim else 1 for axis in range(len(shape))])
    return factor_of


def noise(rng, shape, scale, most, cuts=(), held_as=jnp.bfloat16):
    array = scale * jax.random.normal(rng, shape, jnp.float32)
    if cuts:
        array = array * levels(rng, shape, cuts, -0.22, 0.18)
    return jnp.clip(array, -most, most).astype(held_as)


def gaussian_with(stream_key, dims, width, most, cuts, heavy, kind=jnp.bfloat16):
    drawn = width * jax.random.normal(stream_key, dims, jnp.float32)
    if cuts:
        drawn = drawn * levels(stream_key, dims, cuts, -0.22, 0.18)
    return jnp.clip(spiked(drawn, jax.random.fold_in(stream_key, 3), *heavy), -most, most).astype(kind)


def setup_inputs(seed: int = 0) -> dict:
    key_list = jax.random.split(jax.random.key(seed), 11)
    residual = draw_residual(jax.random.fold_in(key_list[10], 71), 0)
    norm_gain = jnp.clip(1.0 + 0.18 * jax.random.normal(key_list[1], (BLOCKS, D), jnp.float32), 0.099609375, 1.8984375).astype(jnp.bfloat16)
    w_query = noise(key_list[2], (BLOCKS, D, C), D ** -0.5, 0.09375, ((1, 4), (2, 8)))
    w_forget = noise(key_list[3], (BLOCKS, D, C), D ** -0.5, 0.09375, ((1, 4), (2, 8)))
    w_value = noise(key_list[4], (BLOCKS, D, C), D ** -0.5, 0.09375, ((1, 4), (2, 8)))
    w_output_gate = noise(key_list[5], (BLOCKS, D, C), D ** -0.5, 0.09375, ((1, 4), (2, 8)))
    lower_bound = jnp.clip(0.9 * jax.random.uniform(key_list[6], (BLOCKS, C), jnp.float32) ** levels(key_list[6], (BLOCKS, C), ((1, 8),), -0.2, 0.2), 0.0, 0.9)
    head_gain = jnp.clip(1.0 + 0.18 * jax.random.normal(key_list[7], (BLOCKS, C), jnp.float32), 0.099609375, 1.8984375).astype(jnp.bfloat16)
    w_out = gaussian_with(key_list[8], (BLOCKS, C, D), C ** -0.5, 0.125, ((1, 8), (2, 4)), (1, 2, 8, 2.0))
    state = noise(key_list[9], (BLOCKS, BATCH, HEADS, HEAD_DIM, HEAD_DIM), 0.3, 2.4, ((1, 4), (2, 8)), jnp.float32)
    return dict(residual=residual, norm_gain=norm_gain, w_query=w_query, w_forget=w_forget, w_value=w_value, w_output_gate=w_output_gate, lower_bound=lower_bound, head_gain=head_gain, w_out=w_out, state=state)


norm_eps = 1e-06

def one_block(x, gain, w_q, w_f, w_v, w_g, bound, h_gain, w_o, old_state):
    batch = x.shape[0]
    xf = x.astype(jnp.float32)
    scale = lax.rsqrt(lax.optimization_barrier(jnp.mean(xf * xf, axis=1)) + norm_eps)
    scaled_in = (xf * gain.astype(jnp.float32)).astype(jnp.bfloat16)
    rows = scaled_in.reshape(batch, N_DP, D // N_DP).astype(jnp.float32)

    def project(weight):
        blocks = weight.reshape(N_DP, D // N_DP, C).astype(jnp.float32)
        parts = jnp.einsum('bnd,ndc->nbc', rows, blocks)
        parts = lax.optimization_barrier(parts.astype(jnp.bfloat16)).astype(jnp.float32)
        total = lax.optimization_barrier(jnp.sum(parts, axis=0)) * scale[:, None]
        return lax.optimization_barrier(total.astype(jnp.bfloat16)).astype(jnp.float32)
    pq, pf, pv, pg = (project(w_q), project(w_f), project(w_v), project(w_g))
    query = jax.nn.silu(pq).reshape(batch, HEADS, HEAD_DIM)
    forget = (bound + (1.0 - bound) * jax.nn.sigmoid(pf)).reshape(batch, HEADS, HEAD_DIM)
    key = ((1.0 - bound) * jax.nn.sigmoid(-pf)).reshape(batch, HEADS, HEAD_DIM)
    value = pv.reshape(batch, HEADS, HEAD_DIM)
    fresh = forget[..., None] * old_state + key[..., None] * value[:, :, None, :]
    read = jnp.einsum('bhk,bhkv->bhv', query, fresh)
    normed = read * lax.rsqrt(lax.optimization_barrier(jnp.mean(read * read, axis=2, keepdims=True)) + norm_eps)
    normed = normed.reshape(batch, C) * h_gain.astype(jnp.float32)
    hidden = (normed * jax.nn.silu(pg)).astype(jnp.bfloat16)
    mixed = jnp.dot(hidden, w_o, preferred_element_type=jnp.float32)
    return ((xf + mixed).astype(jnp.bfloat16), fresh)

def reference(residual, norm_gain, w_query, w_forget, w_value, w_output_gate, lower_bound, head_gain, w_out, state):
    current = residual
    states = []
    for layer in range(BLOCKS):
        current, fresh = one_block(current, norm_gain[layer], w_query[layer], w_forget[layer], w_value[layer], w_output_gate[layer], lower_bound[layer], head_gain[layer], w_out[layer], state[layer])
        states.append(fresh)
    return (current, jnp.stack(states))
```

```python
import functools

import jax
import jax.numpy as jnp
from jax import lax
from jax.experimental import pallas as pl
from jax.experimental.pallas import tpu as pltpu
from jax.sharding import PartitionSpec as P

D = 4096
HEAD_DIM = 128
BLOCKS = 2


norm_eps = 1e-06


def one_block(x, gain, w_q, w_f, w_v, w_g, bound, h_gain, w_o, old_state):
    xf = x.astype(jnp.float32)
    x_whole, g_whole = (
        lax.all_gather(x, "tp", axis=1, tiled=True),
        lax.all_gather(gain, "tp", axis=1, tiled=True),
    )
    x_wide = x_whole.astype(jnp.float32)
    scaled = (x_wide * g_whole.astype(jnp.float32)).astype(jnp.bfloat16)
    part_q = jnp.dot(scaled, w_q, preferred_element_type=jnp.float32)
    part_f = jnp.dot(scaled, w_f, preferred_element_type=jnp.float32)
    part_v = jnp.dot(scaled, w_v, preferred_element_type=jnp.float32)
    part_g = jnp.dot(scaled, w_g, preferred_element_type=jnp.float32)
    total_sq = lax.psum(jnp.sum(x_wide * x_wide, axis=1), "dp")
    pq, pf, pv, pg = (
        lax.psum_scatter(part_q.astype(jnp.bfloat16), "dp", scatter_dimension=0, tiled=True).astype(
            jnp.float32
        ),
        lax.psum_scatter(part_f.astype(jnp.bfloat16), "dp", scatter_dimension=0, tiled=True).astype(
            jnp.float32
        ),
        lax.psum_scatter(part_v.astype(jnp.bfloat16), "dp", scatter_dimension=0, tiled=True).astype(
            jnp.float32
        ),
        lax.psum_scatter(part_g.astype(jnp.bfloat16), "dp", scatter_dimension=0, tiled=True).astype(
            jnp.float32
        ),
    )
    own = pq.shape[0]
    own_sq = lax.dynamic_slice_in_dim(total_sq, lax.axis_index("dp") * own, own, 0)
    scale = lax.rsqrt(own_sq / D + norm_eps)[:, None]

    def finish(total):
        return lax.optimization_barrier((total * scale).astype(jnp.bfloat16)).astype(jnp.float32)

    pq, pf, pv, pg = (finish(pq), finish(pf), finish(pv), finish(pg))
    heads_here = old_state.shape[1]
    query = jax.nn.silu(pq).reshape(own, heads_here, HEAD_DIM)
    forget = (bound + (1.0 - bound) * jax.nn.sigmoid(pf)).reshape(own, heads_here, HEAD_DIM)
    key = ((1.0 - bound) * jax.nn.sigmoid(-pf)).reshape(own, heads_here, HEAD_DIM)
    value = pv.reshape(own, heads_here, HEAD_DIM)
    fresh = forget[..., None] * old_state + key[..., None] * value[:, :, None, :]
    read = jnp.einsum("bhk,bhkv->bhv", query, fresh)
    normed = read * lax.rsqrt(jnp.mean(read * read, axis=2, keepdims=True) + norm_eps)
    normed = normed.reshape(own, heads_here * HEAD_DIM) * h_gain.astype(jnp.float32)
    hidden = (normed * jax.nn.silu(pg)).astype(jnp.bfloat16)
    terms = jnp.dot(
        lax.all_gather(hidden, "dp", axis=0, tiled=True), w_o, preferred_element_type=jnp.float32
    )
    mixed = lax.psum_scatter(
        terms.astype(jnp.bfloat16), "tp", scatter_dimension=1, tiled=True
    ).astype(jnp.float32)
    return ((xf + mixed).astype(jnp.bfloat16), fresh)


def body(
    residual,
    norm_gain,
    w_query,
    w_forget,
    w_value,
    w_output_gate,
    lower_bound,
    head_gain,
    w_out,
    state,
):
    current = residual
    states = []
    for layer in range(BLOCKS):
        current, fresh = one_block(
            current,
            norm_gain[layer : layer + 1],
            w_query[layer],
            w_forget[layer],
            w_value[layer],
            w_output_gate[layer],
            lower_bound[layer],
            head_gain[layer],
            w_out[layer],
            state[layer],
        )
        states.append(fresh)
    return (current, jnp.stack(states))


LANES = 128
ROLES = 4
PIECES = 8
F32 = jnp.float32
BF16 = jnp.bfloat16


def silu(v):
    return v / (1.0 + jnp.exp(-v))


def sigmoid(v):
    return 1.0 / (1.0 + jnp.exp(-v))


def step_kernel(
    n_tp, n_dp,
    x_hbm, gain_hbm, bound_hbm, h_gain_hbm, wq_hbm, wf_hbm, wv_hbm, wg_hbm, wo_hbm, state_hbm,
    out_ref, s_buf,
    x_ref, raw_gain_ref, bound_ref, raw_h_gain_ref, gain_ref, forget_ref, value_ref, w_buf, wo_buf, xg, gg, scaled, ss_buf, ss_recv, part, pair_recv, mid, part_recv, coef, read, hg,
    terms, pair_terms, mid_terms, terms_recv,
    small_sem, load_sem, x_send, x_recv, g_send, g_recv, ss_send, ss_recv_sem, q_send, q_recv, p_send, p_recv,
    h_send, h_recv, y_send, y_recv, t_send, t_recv,
):
    me_t, me_d = lax.axis_index("tp"), lax.axis_index("dp")
    batch, feats = x_ref.shape
    own = batch // n_dp
    heads = s_buf.shape[2]

    n_z, n_x = n_tp // 2, n_dp // 2
    pair_t = me_t + 1 - 2 * lax.rem(me_t, 2)
    pair_d = me_d + 1 - 2 * lax.rem(me_d, 2)

    def along_z(t, k):
        return lax.rem(t + 2 * k + n_tp, n_tp)

    def along_x(d, k):
        return lax.rem(d + 2 * k + n_dp, n_dp)

    def dp_peer(k):
        return lax.rem(me_d + k, n_dp)

    small = [
        pltpu.make_async_copy(src, dst, small_sem.at[i])
        for i, (src, dst) in enumerate((
            (x_hbm, x_ref), (gain_hbm, raw_gain_ref), (bound_hbm, bound_ref), (h_gain_hbm, raw_h_gain_ref),
        ))
    ]
    for c in small:
        c.start()
    loads = []
    for b in range(BLOCKS):
        group = [
            pltpu.make_async_copy(w.at[b], w_buf.at[b, r], load_sem.at[b, r])
            for r, w in enumerate((wq_hbm, wf_hbm, wv_hbm, wg_hbm))
        ]
        group.append(pltpu.make_async_copy(state_hbm.at[b], s_buf.at[b], load_sem.at[b, 4]))
        group.append(pltpu.make_async_copy(wo_hbm.at[b], wo_buf.at[b], load_sem.at[b, 5]))
        for c in group:
            c.start()
        loads.append(group)

    barrier = pltpu.get_barrier_semaphore()
    for peer in [pair_t] + [along_z(me_t, k) for k in range(1, n_z)]:
        pl.semaphore_signal(barrier, inc=1, device_id={"tp": peer}, device_id_type=pl.DeviceIdType.MESH)
    for k in range(1, n_dp):
        pl.semaphore_signal(barrier, inc=1, device_id={"dp": dp_peer(k)}, device_id_type=pl.DeviceIdType.MESH)
    pl.semaphore_wait(barrier, n_z + n_dp - 1)

    for c in small:
        c.wait()
    gain_ref[pl.ds(0, BLOCKS), :] = raw_gain_ref[...].astype(F32)
    h_gain = raw_h_gain_ref[...].astype(F32)
    sends = []

    def update(b, h):
        lanes = slice(h * HEAD_DIM, (h + 1) * HEAD_DIM)
        f = forget_ref[b, :, lanes].T
        for s in range(own):
            v = value_ref[b, s:s + 1, lanes]
            s_buf[b, s, h] = v + f[:, s:s + 1] * (s_buf[b, s, h] - v)

    def remote(src, dst, send, recv, axis, peer):
        return pltpu.make_async_remote_copy(
            src_ref=src, dst_ref=dst, send_sem=send, recv_sem=recv,
            device_id={axis: peer}, device_id_type=pl.DeviceIdType.MESH,
        )

    def start(*args):
        c = remote(*args)
        c.start()
        sends.append(c)

    for b in range(BLOCKS):
        x_src = x_ref if b == 0 else xg.at[b, me_t]

        def pass_on(x_from, g_from, slot, index, peer):
            if b == 0:
                start(g_from, gg.at[slot], g_send.at[index], g_recv.at[slot], "tp", peer)
            start(x_from, xg.at[b, slot], x_send.at[b, index], x_recv.at[b, slot], "tp", peer)

        def arrived(slot):
            if b == 0:
                remote(gain_ref, gg.at[slot], g_send.at[0], g_recv.at[slot], "tp", pair_t).wait_recv()
            remote(x_src, xg.at[b, slot], x_send.at[b, 0], x_recv.at[b, slot], "tp", pair_t).wait_recv()

        def take(slot, x, g, squares):
            xf = x.astype(F32)
            scaled[:, pl.ds(pl.multiple_of(slot * feats, LANES), feats)] = (xf * g).astype(BF16)
            return squares + xf * xf

        for k in range(1, n_z):
            pass_on(x_src, gain_ref, me_t, k, along_z(me_t, k))
        pass_on(x_src, gain_ref, me_t, n_z, pair_t)
        squares = take(me_t, x_src[...], gain_ref[b:b + 1, :], jnp.zeros((batch, feats), F32))
        arrived(pair_t)
        squares = take(pair_t, xg[b, pair_t], gg[pair_t, b:b + 1, :], squares)
        for k in range(1, n_z):
            src = along_z(me_t, -k)
            arrived(src)
            pass_on(xg.at[b, src], gg.at[src], src, n_z + k, pair_t)
            squares = take(src, xg[b, src], gg[src, b:b + 1, :], squares)
        for k in range(1, n_z):
            src = along_z(pair_t, -k)
            arrived(src)
            squares = take(src, xg[b, src], gg[src, b:b + 1, :], squares)
        ss_buf[b] = jnp.broadcast_to(jnp.sum(squares, axis=1, keepdims=True), (batch, LANES)).reshape(n_dp, own, LANES)
        for k in range(1, n_dp):
            start(ss_buf.at[b, dp_peer(k)], ss_recv.at[b, me_d], ss_send.at[b, k], ss_recv_sem.at[b, me_d], "dp", dp_peer(k))

        def between_chips(r):
            for k in [*range(1, n_x), 0]:
                dst = along_x(me_d, k)
                remote(
                    part.at[b, r, dst], pair_recv.at[b, r, k],
                    q_send.at[b, r, k], q_recv.at[b, r, k], "dp", pair_d,
                ).wait_recv()
                if k:
                    both = part[b, r, dst].astype(F32) + pair_recv[b, r, k].astype(F32)
                    mid[b, r, k] = both.astype(BF16)
                    start(
                        mid.at[b, r, k], part_recv.at[b, r, me_d],
                        p_send.at[b, r, k], p_recv.at[b, r, me_d], "dp", dst,
                    )

        for r in range(ROLES):
            loads[b][r].wait()
            p = jnp.dot(scaled[...], w_buf[b, r], preferred_element_type=F32)
            part[b, r] = p.astype(BF16).reshape(n_dp, own, p.shape[1])
            for k in [*range(1, n_x), 0]:
                start(
                    part.at[b, r, along_x(pair_d, k)], pair_recv.at[b, r, k],
                    q_send.at[b, r, k], q_recv.at[b, r, k], "dp", pair_d,
                )
            if r:
                between_chips(r - 1)
        between_chips(ROLES - 1)
        total_sq = ss_buf[b, me_d]
        for k in range(1, n_dp):
            src = lax.rem(me_d - k + n_dp, n_dp)
            remote(ss_buf.at[b, src], ss_recv.at[b, src], ss_send.at[b, k], ss_recv_sem.at[b, src], "dp", src).wait_recv()
            total_sq = total_sq + ss_recv[b, src]
        scale = lax.rsqrt(total_sq / D + norm_eps)[:, 0:1]
        proj = []
        for r in range(ROLES):
            total = part[b, r, me_d].astype(F32) + pair_recv[b, r, 0].astype(F32)
            for k in range(1, n_x):
                src = along_x(me_d, -k)
                remote(
                    mid.at[b, r, k], part_recv.at[b, r, src],
                    p_send.at[b, r, k], p_recv.at[b, r, src], "dp", src,
                ).wait_recv()
                total = total + part_recv[b, r, src].astype(F32)
            proj.append((total * scale).astype(BF16).astype(F32))
        pq, pf, pv, pg = proj
        bound = bound_ref[b:b + 1, :]
        query = silu(pq)
        forget = bound + (1.0 - bound) * sigmoid(pf)
        key = (1.0 - bound) * sigmoid(-pf)
        forget_ref[b] = forget
        value_ref[b] = pv
        coef[...] = query * forget
        qk = query * key
        loads[b][4].wait()

        @pl.loop(0, heads)
        def _(h):
            lanes = pl.ds(pl.multiple_of(h * HEAD_DIM, HEAD_DIM), HEAD_DIM)
            columns = coef[:, lanes].T
            for s in range(own):
                read[pl.ds(s, 1), lanes] = jnp.sum(columns[:, s:s + 1] * s_buf[b, s, h], axis=0, keepdims=True)

        hidden = []
        for h in range(heads):
            lanes = slice(h * HEAD_DIM, (h + 1) * HEAD_DIM)
            row = read[:, lanes] + jnp.sum(qk[:, lanes], axis=1, keepdims=True) * pv[:, lanes]
            normed = row * lax.rsqrt(jnp.mean(row * row, axis=1, keepdims=True) + norm_eps)
            normed = normed * h_gain[b:b + 1, lanes]
            hg[b, me_d, :, lanes] = (normed * silu(pg[:, lanes])).astype(BF16)
        for k in range(1, n_dp):
            start(hg.at[b, me_d], hg.at[b, me_d], h_send.at[b, k], h_recv.at[b, me_d], "dp", dp_peer(k))
        for h in range(heads // 2):
            update(b, h)
        for k in range(1, n_dp):
            src = lax.rem(me_d - k + n_dp, n_dp)
            remote(hg.at[b, src], hg.at[b, src], h_send.at[b, k], h_recv.at[b, src], "dp", src).wait_recv()
        loads[b][5].wait()
        everyone = hg[b].reshape(batch, hg.shape[3])

        def piece(dst):
            lanes = pl.ds(pl.multiple_of(dst * feats, LANES), feats)
            return jnp.dot(everyone, wo_buf[b, :, lanes], preferred_element_type=F32)

        order = [*range(1, n_z), 0]
        for k in order:
            terms[b, k] = piece(along_z(pair_t, k)).astype(BF16)
            start(terms.at[b, k], pair_terms.at[b, k], y_send.at[b, k], y_recv.at[b, k], "tp", pair_t)
        for h in range(heads // 2, heads):
            update(b, h)
        for k in order:
            total = piece(along_z(me_t, k))
            remote(terms.at[b, k], pair_terms.at[b, k], y_send.at[b, k], y_recv.at[b, k], "tp", pair_t).wait_recv()
            total = total + pair_terms[b, k].astype(F32)
            if k:
                mid_terms[b, k] = total.astype(BF16)
                start(
                    mid_terms.at[b, k], terms_recv.at[b, me_t], t_send.at[b, k], t_recv.at[b, me_t],
                    "tp", along_z(me_t, k),
                )
        for k in range(1, n_z):
            src = along_z(me_t, -k)
            remote(mid_terms.at[b, k], terms_recv.at[b, src], t_send.at[b, k], t_recv.at[b, src], "tp", src).wait_recv()
            total = total + terms_recv[b, src].astype(F32)
        x_next = (x_src[...].astype(F32) + total).astype(BF16)
        if b + 1 < BLOCKS:
            xg[b + 1, me_t] = x_next
        else:
            out_ref[...] = x_next
    for c in sends:
        c.wait_send()


def flush_kernel(x_ref, state_ref, out_ref, new_ref, sem):
    blocks, rows = state_ref.shape[:2]
    copies = [pltpu.make_async_copy(x_ref, out_ref, sem.at[0, 0])]
    for b in range(blocks):
        for c in range(PIECES):
            part = pl.ds(c * (rows // PIECES), rows // PIECES)
            copies.append(pltpu.make_async_copy(state_ref.at[b, part], new_ref.at[b, part], sem.at[1 + b, c]))
    for c in copies:
        c.start()
    for c in copies:
        c.wait()


def fast_body(
    n_tp, n_dp, residual, norm_gain, w_query, w_forget, w_value, w_output_gate, lower_bound, head_gain, w_out, state
):
    batch, feats = residual.shape
    rows, cols = w_query.shape[1:]
    own, heads = state.shape[1:3]
    vmem = pl.BlockSpec(memory_space=pltpu.VMEM)
    hbm = pl.BlockSpec(memory_space=pltpu.HBM)
    dma = pltpu.SemaphoreType.DMA
    current, fresh = pl.pallas_call(
        functools.partial(step_kernel, n_tp, n_dp),
        out_shape=(pltpu.VMEM((batch, feats), BF16), pltpu.VMEM(state.shape, F32)),
        in_specs=[hbm] * 10,
        out_specs=(vmem,) * 2,
        scratch_shapes=[
            pltpu.VMEM((batch, feats), BF16),
            pltpu.VMEM(norm_gain.shape, norm_gain.dtype),
            pltpu.VMEM(lower_bound.shape, lower_bound.dtype),
            pltpu.VMEM(head_gain.shape, head_gain.dtype),
            pltpu.VMEM((8, feats), F32),
            pltpu.VMEM((BLOCKS, own, cols), F32),
            pltpu.VMEM((BLOCKS, own, cols), F32),
            pltpu.VMEM((BLOCKS, ROLES, rows, cols), BF16),
            pltpu.VMEM((BLOCKS, *w_out.shape[1:]), BF16),
            pltpu.VMEM((BLOCKS, n_tp, batch, feats), BF16),
            pltpu.VMEM((n_tp, 8, feats), F32),
            pltpu.VMEM((batch, rows), BF16),
            pltpu.VMEM((BLOCKS, n_dp, own, LANES), F32),
            pltpu.VMEM((BLOCKS, n_dp, own, LANES), F32),
            pltpu.VMEM((BLOCKS, ROLES, n_dp, own, cols), BF16),
            pltpu.VMEM((BLOCKS, ROLES, n_dp // 2, own, cols), BF16),
            pltpu.VMEM((BLOCKS, ROLES, n_dp // 2, own, cols), BF16),
            pltpu.VMEM((BLOCKS, ROLES, n_dp, own, cols), BF16),
            pltpu.VMEM((own, cols), F32),
            pltpu.VMEM((own, cols), F32),
            pltpu.VMEM((BLOCKS, n_dp, own, cols), BF16),
            pltpu.VMEM((BLOCKS, n_tp // 2, batch, feats), BF16),
            pltpu.VMEM((BLOCKS, n_tp // 2, batch, feats), BF16),
            pltpu.VMEM((BLOCKS, n_tp // 2, batch, feats), BF16),
            pltpu.VMEM((BLOCKS, n_tp, batch, feats), BF16),
            dma((4,)),
            dma((BLOCKS, 6)),
            dma((BLOCKS, n_tp)), dma((BLOCKS, n_tp)),
            dma((n_tp,)), dma((n_tp,)),
            dma((BLOCKS, n_dp)), dma((BLOCKS, n_dp)),
            dma((BLOCKS, ROLES, n_dp // 2)), dma((BLOCKS, ROLES, n_dp // 2)),
            dma((BLOCKS, ROLES, n_dp)), dma((BLOCKS, ROLES, n_dp)),
            dma((BLOCKS, n_dp)), dma((BLOCKS, n_dp)),
            dma((BLOCKS, n_tp // 2)), dma((BLOCKS, n_tp // 2)),
            dma((BLOCKS, n_tp)), dma((BLOCKS, n_tp)),
        ],
        compiler_params=pltpu.CompilerParams(
            collective_id=0, has_side_effects=True, vmem_limit_bytes=32 * 1024 * 1024
        ),
        name="recurrent_step",
    )(
        *(
            pltpu.with_memory_space_constraint(a, pltpu.HBM)
            for a in (
                residual, norm_gain, lower_bound, head_gain, w_query, w_forget, w_value, w_output_gate, w_out, state
            )
        )
    )
    return tuple(pl.pallas_call(
        flush_kernel,
        out_shape=(jax.ShapeDtypeStruct((batch, feats), BF16), jax.ShapeDtypeStruct(state.shape, F32)),
        in_specs=[vmem] * 2,
        out_specs=(hbm,) * 2,
        scratch_shapes=[dma((1 + BLOCKS, PIECES))],
        compiler_params=pltpu.CompilerParams(vmem_limit_bytes=4 * 1024 * 1024),
        name="flush",
    )(
        pltpu.with_memory_space_constraint(current, pltpu.VMEM),
        pltpu.with_memory_space_constraint(fresh, pltpu.VMEM),
    ))


def solution(mesh):
    placed = (
        P(None, ("dp", "tp")),
        P(None, ("dp", "tp")),
        P(None, "dp", "tp"),
        P(None, "dp", "tp"),
        P(None, "dp", "tp"),
        P(None, "dp", "tp"),
        P(None, "tp"),
        P(None, "tp"),
        P(None, "tp", "dp"),
        P(None, "dp", "tp", None, None),
    )
    n_tp, n_dp = mesh.shape["tp"], mesh.shape["dp"]
    whole_tiles = D % (n_tp * n_dp * LANES) == 0 and n_tp % 2 == 0 and n_dp % 2 == 0
    return jax.shard_map(
        functools.partial(fast_body, n_tp, n_dp) if whole_tiles else body,
        mesh=mesh,
        in_specs=placed,
        out_specs=(P(None, ("dp", "tp")), P(None, "dp", "tp", None, None)),
        check_vma=False,
    )
```

```python
import functools

import jax
import jax.numpy as jnp
from jax import lax
from jax.experimental import pallas as pl
from jax.experimental.pallas import tpu as pltpu
from jax.sharding import PartitionSpec as P

D = 4096
HEAD_DIM = 128
BLOCKS = 2


norm_eps = 1e-06


def one_block(x, gain, w_q, w_f, w_v, w_g, bound, h_gain, w_o, old_state):
    xf = x.astype(jnp.float32)
    x_whole, g_whole = (
        lax.all_gather(x, "tp", axis=1, tiled=True),
        lax.all_gather(gain, "tp", axis=1, tiled=True),
    )
    x_wide = x_whole.astype(jnp.float32)
    scaled = (x_wide * g_whole.astype(jnp.float32)).astype(jnp.bfloat16)
    part_q = jnp.dot(scaled, w_q, preferred_element_type=jnp.float32)
    part_f = jnp.dot(scaled, w_f, preferred_element_type=jnp.float32)
    part_v = jnp.dot(scaled, w_v, preferred_element_type=jnp.float32)
    part_g = jnp.dot(scaled, w_g, preferred_element_type=jnp.float32)
    total_sq = lax.psum(jnp.sum(x_wide * x_wide, axis=1), "dp")
    pq, pf, pv, pg = (
        lax.psum_scatter(part_q.astype(jnp.bfloat16), "dp", scatter_dimension=0, tiled=True).astype(
            jnp.float32
        ),
        lax.psum_scatter(part_f.astype(jnp.bfloat16), "dp", scatter_dimension=0, tiled=True).astype(
            jnp.float32
        ),
        lax.psum_scatter(part_v.astype(jnp.bfloat16), "dp", scatter_dimension=0, tiled=True).astype(
            jnp.float32
        ),
        lax.psum_scatter(part_g.astype(jnp.bfloat16), "dp", scatter_dimension=0, tiled=True).astype(
            jnp.float32
        ),
    )
    own = pq.shape[0]
    own_sq = lax.dynamic_slice_in_dim(total_sq, lax.axis_index("dp") * own, own, 0)
    scale = lax.rsqrt(own_sq / D + norm_eps)[:, None]

    def finish(total):
        return lax.optimization_barrier((total * scale).astype(jnp.bfloat16)).astype(jnp.float32)

    pq, pf, pv, pg = (finish(pq), finish(pf), finish(pv), finish(pg))
    heads_here = old_state.shape[1]
    query = jax.nn.silu(pq).reshape(own, heads_here, HEAD_DIM)
    forget = (bound + (1.0 - bound) * jax.nn.sigmoid(pf)).reshape(own, heads_here, HEAD_DIM)
    key = ((1.0 - bound) * jax.nn.sigmoid(-pf)).reshape(own, heads_here, HEAD_DIM)
    value = pv.reshape(own, heads_here, HEAD_DIM)
    fresh = forget[..., None] * old_state + key[..., None] * value[:, :, None, :]
    read = jnp.einsum("bhk,bhkv->bhv", query, fresh)
    normed = read * lax.rsqrt(jnp.mean(read * read, axis=2, keepdims=True) + norm_eps)
    normed = normed.reshape(own, heads_here * HEAD_DIM) * h_gain.astype(jnp.float32)
    hidden = (normed * jax.nn.silu(pg)).astype(jnp.bfloat16)
    terms = jnp.dot(
        lax.all_gather(hidden, "dp", axis=0, tiled=True), w_o, preferred_element_type=jnp.float32
    )
    mixed = lax.psum_scatter(
        terms.astype(jnp.bfloat16), "tp", scatter_dimension=1, tiled=True
    ).astype(jnp.float32)
    return ((xf + mixed).astype(jnp.bfloat16), fresh)


def body(
    residual,
    norm_gain,
    w_query,
    w_forget,
    w_value,
    w_output_gate,
    lower_bound,
    head_gain,
    w_out,
    state,
):
    current = residual
    states = []
    for layer in range(BLOCKS):
        current, fresh = one_block(
            current,
            norm_gain[layer : layer + 1],
            w_query[layer],
            w_forget[layer],
            w_value[layer],
            w_output_gate[layer],
            lower_bound[layer],
            head_gain[layer],
            w_out[layer],
            state[layer],
        )
        states.append(fresh)
    return (current, jnp.stack(states))


LANES = 128
ROLES = 4
PIECES = 8
HALVES = 2
F32 = jnp.float32
BF16 = jnp.bfloat16


def silu(v):
    return v / (1.0 + jnp.exp(-v))


def sigmoid(v):
    return 1.0 / (1.0 + jnp.exp(-v))


def flip(v, bit):
    return v + bit * (1 - 2 * lax.rem(lax.div(v, bit), 2))


def ranked(z, n_z):
    if n_z == 4:
        upper = lax.div(z, 2)
        return [3 - 3 * upper, 2 - upper, flip(z, 1)]
    others = []
    for k in range(n_z - 1, 0, -1):
        other, bit = z, 1
        while bit <= k:
            other = flip(other, bit) if k & bit else other
            bit *= 2
        others.append(other)
    return others


def step_kernel(
    n_tp, n_dp,
    x_hbm, gain_hbm, bound_hbm, h_gain_hbm, wq_hbm, wf_hbm, wv_hbm, wg_hbm, wo_hbm, state_hbm,
    out_ref, s_buf,
    raw_gain_ref, bound_ref, raw_h_gain_ref, gain_ref, forget_ref, value_ref, w_buf, wo_buf, xg, gg, scaled, sq,
    ss_buf, ss_recv, part, pair_recv, mid, part_recv, coef, read, hg, acc, terms, pair_terms, mid_terms, terms_recv,
    small_sem, load_sem, x_send, x_recv, g_send, g_recv, ss_send, ss_recv_sem, q_send, q_recv, p_send, p_recv,
    h_send, h_recv, y_send, y_recv, t_send, t_recv,
):
    me_t, me_d = lax.axis_index("tp"), lax.axis_index("dp")
    batch, feats = x_hbm.shape
    own, heads = s_buf.shape[1:3]
    rows, cols = w_buf.shape[2:]
    half, many = own // HALVES, batch // HALVES

    n_z, n_x = n_tp // 2, n_dp // 2
    me_y, me_z = lax.rem(me_t, 2), lax.div(me_t, 2)
    pair_t, pair_d = flip(me_t, 1), flip(me_d, 1)
    peers = ranked(me_z, n_z)
    near_first = [*reversed([*enumerate(peers)])]

    def along_x(d, k):
        return lax.rem(d + 2 * k + n_dp, n_dp)

    def dp_peer(k):
        return lax.rem(me_d + k, n_dp)

    def columns_of(slot):
        return pl.ds(pl.multiple_of(slot * feats, LANES), feats)

    small = []
    for h in range(HALVES):
        for d in range(n_dp):
            small.append((x_hbm.at[pl.ds(d * own + h * half, half)], xg.at[0, h, me_t, pl.ds(d * half, half)]))
    small += [(gain_hbm, raw_gain_ref), (bound_hbm, bound_ref), (h_gain_hbm, raw_h_gain_ref)]
    small = [pltpu.make_async_copy(src, dst, small_sem.at[i]) for i, (src, dst) in enumerate(small)]
    for c in small:
        c.start()

    barrier = pltpu.get_barrier_semaphore()
    for peer in [pair_t] + [2 * z + me_y for z in peers]:
        pl.semaphore_signal(barrier, inc=1, device_id={"tp": peer}, device_id_type=pl.DeviceIdType.MESH)
    for k in range(1, n_dp):
        pl.semaphore_signal(barrier, inc=1, device_id={"dp": dp_peer(k)}, device_id_type=pl.DeviceIdType.MESH)
    for c in small:
        c.wait()
    gain_ref[pl.ds(0, BLOCKS), :] = raw_gain_ref[...].astype(F32)
    h_gain = raw_h_gain_ref[...].astype(F32)

    loads = []
    for b in range(BLOCKS):
        group = [
            pltpu.make_async_copy(w.at[b], w_buf.at[b, r], load_sem.at[b, r])
            for r, w in enumerate((wq_hbm, wf_hbm, wv_hbm, wg_hbm))
        ]
        group.append(pltpu.make_async_copy(state_hbm.at[b], s_buf.at[b], load_sem.at[b, ROLES]))
        group.append(pltpu.make_async_copy(wo_hbm.at[b], wo_buf.at[b], load_sem.at[b, ROLES + 1]))
        loads.append(group)
    for c in loads[0][:ROLES]:
        c.start()
    pl.semaphore_wait(barrier, n_z + n_dp - 1)

    sends = []

    def remote(src, dst, send, recv, axis, peer):
        return pltpu.make_async_remote_copy(
            src_ref=src, dst_ref=dst, send_sem=send, recv_sem=recv,
            device_id={axis: peer}, device_id_type=pl.DeviceIdType.MESH,
        )

    def start(*args):
        c = remote(*args)
        c.start()
        sends.append(c)

    def pass_on(b, h, slot, index, peer):
        if b == 0 and h == 0:
            start(gain_ref if slot is me_t else gg.at[slot], gg.at[slot], g_send.at[index], g_recv.at[slot], "tp", peer)
        block = xg.at[b, h, slot]
        start(block, block, x_send.at[b, h, index], x_recv.at[b, h, slot], "tp", peer)

    def arrived(b, h, slot):
        if b == 0 and h == 0:
            remote(gg.at[slot], gg.at[slot], g_send.at[0], g_recv.at[slot], "tp", pair_t).wait_recv()
        block = xg.at[b, h, slot]
        remote(block, block, x_send.at[b, h, 0], x_recv.at[b, h, slot], "tp", pair_t).wait_recv()

    def take(b, h, slot):
        xf = xg[b, h, slot].astype(F32)
        g = (gain_ref if slot is me_t else gg.at[slot])[b:b + 1, :]
        scaled[h, :, columns_of(slot)] = (xf * g).astype(BF16)
        sq[h] = xf * xf if slot is me_t else sq[h] + xf * xf

    def gather_send(b, h):
        for j, z in enumerate(peers):
            pass_on(b, h, me_t, j, 2 * z + me_y)
        pass_on(b, h, me_t, n_z - 1, pair_t)
        take(b, h, me_t)

    def gather_along_z(b, h):
        for j, z in near_first:
            slot = 2 * z + me_y
            arrived(b, h, slot)
            pass_on(b, h, slot, n_z + j, pair_t)
            take(b, h, slot)

    def gather_along_y(b, h):
        for slot in [pair_t] + [2 * z + 1 - me_y for _, z in near_first]:
            arrived(b, h, slot)
            take(b, h, slot)
        total = jnp.sum(sq[h], axis=1, keepdims=True)
        ss_buf[b, h] = jnp.broadcast_to(total, (many, LANES)).reshape(n_dp, half, LANES)
        for k in range(1, n_dp):
            start(
                ss_buf.at[b, h, dp_peer(k)], ss_recv.at[b, h, me_d],
                ss_send.at[b, h, k], ss_recv_sem.at[b, h, me_d], "dp", dp_peer(k),
            )

    def project(b, h, r):
        if h == 0:
            loads[b][r].wait()
        p = jnp.dot(scaled[h], w_buf[b, r], preferred_element_type=F32)
        part[b, h, r] = p.astype(BF16).reshape(n_dp, half, cols)
        for k in [*range(1, n_x), 0]:
            start(
                part.at[b, h, r, along_x(pair_d, k)], pair_recv.at[b, h, r, k],
                q_send.at[b, h, r, k], q_recv.at[b, h, r, k], "dp", pair_d,
            )

    def between_chips(b, h, r):
        for k in [*range(1, n_x), 0]:
            dst = along_x(me_d, k)
            remote(
                part.at[b, h, r, dst], pair_recv.at[b, h, r, k],
                q_send.at[b, h, r, k], q_recv.at[b, h, r, k], "dp", pair_d,
            ).wait_recv()
            if k:
                both = part[b, h, r, dst].astype(F32) + pair_recv[b, h, r, k].astype(F32)
                mid[b, h, r, k] = both.astype(BF16)
                start(
                    mid.at[b, h, r, k], part_recv.at[b, h, r, me_d],
                    p_send.at[b, h, r, k], p_recv.at[b, h, r, me_d], "dp", dst,
                )

    def read_out(b, h):
        total_sq = ss_buf[b, h, me_d]
        for k in range(1, n_dp):
            src = lax.rem(me_d - k + n_dp, n_dp)
            remote(
                ss_buf.at[b, h, src], ss_recv.at[b, h, src],
                ss_send.at[b, h, k], ss_recv_sem.at[b, h, src], "dp", src,
            ).wait_recv()
            total_sq = total_sq + ss_recv[b, h, src]
        scale = lax.rsqrt(total_sq / (rows * n_dp) + norm_eps)[:, 0:1]
        proj = []
        for r in range(ROLES):
            total = part[b, h, r, me_d].astype(F32) + pair_recv[b, h, r, 0].astype(F32)
            for k in range(1, n_x):
                src = along_x(me_d, -k)
                remote(
                    mid.at[b, h, r, k], part_recv.at[b, h, r, src],
                    p_send.at[b, h, r, k], p_recv.at[b, h, r, src], "dp", src,
                ).wait_recv()
                total = total + part_recv[b, h, r, src].astype(F32)
            proj.append((total * scale).astype(BF16).astype(F32))
        pq, pf, pv, pg = proj
        bound = bound_ref[b:b + 1, :]
        query = silu(pq)
        forget = bound + (1.0 - bound) * sigmoid(pf)
        key = (1.0 - bound) * sigmoid(-pf)
        forget_ref[b, h] = forget
        value_ref[b, h] = pv
        coef[h] = query * forget
        qk = query * key
        if h == 0:
            loads[b][ROLES].wait()

        @pl.loop(0, heads)
        def _(head):
            lanes = pl.ds(pl.multiple_of(head * HEAD_DIM, HEAD_DIM), HEAD_DIM)
            factors = coef[h, :, lanes]
            for s in range(half):
                sums = jnp.dot(factors, s_buf[b, h * half + s, head], preferred_element_type=F32)
                read[h, pl.ds(s, 1), lanes] = sums[s:s + 1]

        for head in range(heads):
            lanes = slice(head * HEAD_DIM, (head + 1) * HEAD_DIM)
            row = read[h, :, lanes] + jnp.sum(qk[:, lanes], axis=1, keepdims=True) * pv[:, lanes]
            normed = row * lax.rsqrt(jnp.mean(row * row, axis=1, keepdims=True) + norm_eps)
            normed = normed * h_gain[b:b + 1, lanes]
            hg[b, h, me_d, :, lanes] = (normed * silu(pg[:, lanes])).astype(BF16)
        for k in range(1, n_dp):
            mine = hg.at[b, h, me_d]
            start(mine, mine, h_send.at[b, h, k], h_recv.at[b, h, me_d], "dp", dp_peer(k))

    def mix(b, h):
        for k in range(1, n_dp):
            src = lax.rem(me_d - k + n_dp, n_dp)
            theirs = hg.at[b, h, src]
            remote(theirs, theirs, h_send.at[b, h, k], h_recv.at[b, h, src], "dp", src).wait_recv()
        if h == 0:
            loads[b][ROLES + 1].wait()
        everyone = hg[b, h].reshape(many, cols)
        acc[h] = jnp.dot(everyone, wo_buf[b], preferred_element_type=F32)
        for j, z in enumerate([*peers, me_z]):
            terms[b, h, j] = acc[h, :, columns_of(2 * z + 1 - me_y)].astype(BF16)
            start(terms.at[b, h, j], pair_terms.at[b, h, j], y_send.at[b, h, j], y_recv.at[b, h, j], "tp", pair_t)

    def reduce_along_z(b, h):
        for j, z in enumerate([*peers, me_z]):
            remote(
                terms.at[b, h, j], pair_terms.at[b, h, j], y_send.at[b, h, j], y_recv.at[b, h, j], "tp", pair_t
            ).wait_recv()
            if j < n_z - 1:
                mid_terms[b, h, j] = (acc[h, :, columns_of(2 * z + me_y)] + pair_terms[b, h, j].astype(F32)).astype(BF16)
                start(
                    mid_terms.at[b, h, j], terms_recv.at[b, h, me_z], t_send.at[b, h, j], t_recv.at[b, h, me_z],
                    "tp", 2 * z + me_y,
                )

    def residual(b, h):
        total = acc[h, :, columns_of(me_t)] + pair_terms[b, h, n_z - 1].astype(F32)
        for j, z in near_first:
            remote(
                mid_terms.at[b, h, j], terms_recv.at[b, h, z], t_send.at[b, h, j], t_recv.at[b, h, z],
                "tp", 2 * z + me_y,
            ).wait_recv()
            total = total + terms_recv[b, h, z].astype(F32)
        x_next = (xg[b, h, me_t].astype(F32) + total).astype(BF16)
        if b + 1 < BLOCKS:
            xg[b + 1, h, me_t] = x_next
            gather_send(b + 1, h)
        else:
            for d in range(n_dp):
                out_ref[pl.ds(d * own + h * half, half), :] = x_next[d * half:(d + 1) * half]

    pending = []

    def update(count):
        for b, h, head in pending[:count]:
            lanes = slice(head * HEAD_DIM, (head + 1) * HEAD_DIM)
            f = forget_ref[b, h, :, lanes].T
            for s in range(half):
                v = value_ref[b, h, s:s + 1, lanes]
                old = s_buf[b, h * half + s, head]
                s_buf[b, h * half + s, head] = v + f[:, s:s + 1] * (old - v)
        del pending[:count]

    both = range(HALVES)
    for h in both:
        gather_send(0, h)
    for c in loads[0][ROLES:]:
        c.start()
    for b in range(BLOCKS):
        for h in both:
            gather_along_z(b, h)
        for h in both:
            gather_along_y(b, h)
            for r in range(ROLES):
                project(b, h, r)
            if h:
                for r in range(ROLES):
                    between_chips(b, h - 1, r)
        for r in range(ROLES):
            between_chips(b, HALVES - 1, r)
        if b + 1 < BLOCKS:
            for c in loads[b + 1]:
                c.start()
        for h in both:
            read_out(b, h)
            pending += [(b, h, head) for head in range(heads)]
        units = len(pending)
        for h in both:
            mix(b, h)
        update(units // 4)
        for h in both:
            reduce_along_z(b, h)
        update(units // 2 if b + 1 < BLOCKS else units)
        for h in both:
            residual(b, h)
        update(units)
    for c in sends:
        c.wait_send()


def flush_kernel(x_ref, state_ref, out_ref, new_ref, sem):
    blocks, rows = state_ref.shape[:2]
    copies = [pltpu.make_async_copy(x_ref, out_ref, sem.at[0, 0])]
    for b in range(blocks):
        for c in range(PIECES):
            part = pl.ds(c * (rows // PIECES), rows // PIECES)
            copies.append(pltpu.make_async_copy(state_ref.at[b, part], new_ref.at[b, part], sem.at[1 + b, c]))
    for c in copies:
        c.start()
    for c in copies:
        c.wait()


def fast_body(
    n_tp, n_dp, residual, norm_gain, w_query, w_forget, w_value, w_output_gate, lower_bound, head_gain, w_out, state
):
    batch, feats = residual.shape
    rows, cols = w_query.shape[1:]
    own, heads = state.shape[1:3]
    half, many, n_z, each = own // HALVES, batch // HALVES, n_tp // 2, (BLOCKS, HALVES)
    vmem = pl.BlockSpec(memory_space=pltpu.VMEM)
    hbm = pl.BlockSpec(memory_space=pltpu.HBM)
    dma = pltpu.SemaphoreType.DMA
    current, fresh = pl.pallas_call(
        functools.partial(step_kernel, n_tp, n_dp),
        out_shape=(pltpu.VMEM((batch, feats), BF16), pltpu.VMEM(state.shape, F32)),
        in_specs=[hbm] * 10,
        out_specs=(vmem,) * 2,
        scratch_shapes=[
            pltpu.VMEM(norm_gain.shape, norm_gain.dtype),
            pltpu.VMEM(lower_bound.shape, lower_bound.dtype),
            pltpu.VMEM(head_gain.shape, head_gain.dtype),
            pltpu.VMEM((8, feats), F32),
            pltpu.VMEM((*each, half, cols), F32),
            pltpu.VMEM((*each, half, cols), F32),
            pltpu.VMEM((BLOCKS, ROLES, rows, cols), BF16),
            pltpu.VMEM((BLOCKS, *w_out.shape[1:]), BF16),
            pltpu.VMEM((*each, n_tp, many, feats), BF16),
            pltpu.VMEM((n_tp, 8, feats), F32),
            pltpu.VMEM((HALVES, many, rows), BF16),
            pltpu.VMEM((HALVES, many, feats), F32),
            pltpu.VMEM((*each, n_dp, half, LANES), F32),
            pltpu.VMEM((*each, n_dp, half, LANES), F32),
            pltpu.VMEM((*each, ROLES, n_dp, half, cols), BF16),
            pltpu.VMEM((*each, ROLES, n_dp // 2, half, cols), BF16),
            pltpu.VMEM((*each, ROLES, n_dp // 2, half, cols), BF16),
            pltpu.VMEM((*each, ROLES, n_dp, half, cols), BF16),
            pltpu.VMEM((HALVES, half, cols), F32),
            pltpu.VMEM((HALVES, half, cols), F32),
            pltpu.VMEM((*each, n_dp, half, cols), BF16),
            pltpu.VMEM((HALVES, many, n_tp * feats), F32),
            pltpu.VMEM((*each, n_z, many, feats), BF16),
            pltpu.VMEM((*each, n_z, many, feats), BF16),
            pltpu.VMEM((*each, n_z, many, feats), BF16),
            pltpu.VMEM((*each, n_z, many, feats), BF16),
            dma((HALVES * n_dp + 3,)),
            dma((BLOCKS, ROLES + 2)),
            dma((*each, n_tp)), dma((*each, n_tp)),
            dma((n_tp,)), dma((n_tp,)),
            dma((*each, n_dp)), dma((*each, n_dp)),
            dma((*each, ROLES, n_dp // 2)), dma((*each, ROLES, n_dp // 2)),
            dma((*each, ROLES, n_dp)), dma((*each, ROLES, n_dp)),
            dma((*each, n_dp)), dma((*each, n_dp)),
            dma((*each, n_z)), dma((*each, n_z)),
            dma((*each, n_z)), dma((*each, n_z)),
        ],
        compiler_params=pltpu.CompilerParams(
            collective_id=0, has_side_effects=True, vmem_limit_bytes=32 * 1024 * 1024
        ),
        name="recurrent_step",
    )(
        *(
            pltpu.with_memory_space_constraint(a, pltpu.HBM)
            for a in (
                residual, norm_gain, lower_bound, head_gain, w_query, w_forget, w_value, w_output_gate, w_out, state
            )
        )
    )
    return tuple(pl.pallas_call(
        flush_kernel,
        out_shape=(jax.ShapeDtypeStruct((batch, feats), BF16), jax.ShapeDtypeStruct(state.shape, F32)),
        in_specs=[vmem] * 2,
        out_specs=(hbm,) * 2,
        scratch_shapes=[dma((1 + BLOCKS, PIECES))],
        compiler_params=pltpu.CompilerParams(vmem_limit_bytes=4 * 1024 * 1024),
        name="flush",
    )(
        pltpu.with_memory_space_constraint(current, pltpu.VMEM),
        pltpu.with_memory_space_constraint(fresh, pltpu.VMEM),
    ))


def solution(mesh):
    placed = (
        P(None, ("dp", "tp")),
        P(None, ("dp", "tp")),
        P(None, "dp", "tp"),
        P(None, "dp", "tp"),
        P(None, "dp", "tp"),
        P(None, "dp", "tp"),
        P(None, "tp"),
        P(None, "tp"),
        P(None, "tp", "dp"),
        P(None, "dp", "tp", None, None),
    )
    n_tp, n_dp = mesh.shape["tp"], mesh.shape["dp"]
    whole_tiles = D % (n_tp * n_dp * LANES) == 0 and n_tp in (2, 4, 8, 16) and n_dp % 2 == 0
    return jax.shard_map(
        functools.partial(fast_body, n_tp, n_dp) if whole_tiles else body,
        mesh=mesh,
        in_specs=placed,
        out_specs=(P(None, ("dp", "tp")), P(None, "dp", "tp", None, None)),
        check_vma=False,
    )
```
